256 devices in a mesh: grp: 2 (over y), sp: 32 (over z, core), tp: 4 (over x).
Axes of the slice: x: 4, y: 2, z: 16, core: 2. Of those that a mesh axis runs over, the one named last changes fastest.
The devices are a block of a 4x16x16 slice.
Arguments:
- query_wide: bfloat16 [32768, 1024], P(('grp', 'sp'), 'tp'), parts along dimension 0, may hold values from -6 to 6
- key_wide: bfloat16 [32768, 1024], P(('grp', 'sp'), 'tp'), parts along dimension 0, may hold values from -6 to 6
- value_wide: bfloat16 [32768, 1024], P(('grp', 'sp'), 'tp'), parts along dimension 0, may hold values from -6 to 6
- decay_wide: float32 [32768, 8], P(('grp', 'sp'), 'tp'), parts along dimension 0, may hold values from -2 to 0, as said below
- query_narrow: bfloat16 [32768, 1024], P(('grp', 'sp'), 'tp'), parts along dimension 0, may hold values from -6 to 6
- key_narrow: bfloat16 [32768, 1024], P(('grp', 'sp'), 'tp'), parts along dimension 0, may hold values from -6 to 6
- value_narrow: bfloat16 [32768, 1024], P(('grp', 'sp'), 'tp'), parts along dimension 0, may hold values from -6 to 6
- decay_narrow: float32 [32768, 16], P(('grp', 'sp'), 'tp'), parts along dimension 0, may hold values from -2 to 0, as said below
- residual: bfloat16 [32768, 2048], P(('grp', 'sp', 'tp')), parts along dimension 0, may hold values from -6 to 6
- out_wide: bfloat16 [1024, 2048], P('tp'), may hold values from -0.125 to 0.125
- out_narrow: bfloat16 [1024, 2048], P('tp'), may hold values from -0.125 to 0.125
- norm_gain: float32 [2048], replicated, may hold values from 0.1 to 1.9
- routes: int32 [32768, 2], P(('grp', 'sp', 'tp')), parts along dimension 0, may hold values from 0 to 31, all different within a row; in each aligned block of 128 rows (0 to 127, 128 to 255, ...) at most 12 rows name the same one
- route_weights: float32 [32768, 2], P(('grp', 'sp', 'tp')), parts along dimension 0, may hold values from 0.1 to 1
- expert_gate: bfloat16 [32, 2048, 2048], P('sp', None, 'tp'), may hold values from -0.375 to 0.375
- expert_up: bfloat16 [32, 2048, 2048], P('sp', None, 'tp'), may hold values from -0.375 to 0.375
- expert_down: bfloat16 [32, 2048, 2048], P('sp', 'tp'), may hold values from -0.03125 to 0.03125
Outputs:
- layer_out: bfloat16 [32768, 2048], P(('grp', 'sp', 'tp')), parts along dimension 0
The draws below stay inside these ranges and needn't reach their ends.
There are 2 independent parts, one for each index of `grp`. The reference program is written for one: setup_inputs(seed, part) draws one part's arguments, and reference() takes and returns one part's arrays. A program takes and returns all parts, laid end to end along the dimension named above; an argument that names none is the same for every part. Nothing has to cross between parts.
Inputs may be any that keep to these rules, and one draw needn't show every extreme that they name: `decay_wide`: every entry is negative. `decay_narrow`: every entry is negative. `routes`: each row names 2 different experts; on the rows of one device no expert is named more than 12 times, a bound that some block reaches.
All inputs are finite; a program needn't handle non-finite values.
Results may differ from the reference program's by a relative error of at most 0.018.
Values may be sent and summed in bfloat16 or wider, within the bound.
No kernel may reach another device: no remote copies, remote signals or barrier semaphores. Data moves between devices by JAX's collectives and lax.ppermute only.
A program may use at most 128 MiB of HBM per device.

```python
import math
import jax
import jax.numpy as jnp
import numpy as np
from jax import lax

D = 2048
HEADS_WIDE = 8
HEAD_WIDE = 128
HEADS_NARROW = 16
HEAD_NARROW = 64
FF = 2048
TOP_K = 2
TOK_DEV = 512
STEP_COUNT_FULL = 16384
EXPERTS = 32
ROWS_DEV = 128
CAPACITY = 12
N_SP = 32
N_TP = 4


def decay_draw(key, attention_group_count):
    lookup_vectors = jax.random.split(key, 7)
    fast_share = 0.5
    fast_heads = jax.random.uniform(lookup_vectors[0], (attention_group_count,), jnp.float32) < fast_share
    fast_rate = jax.random.uniform(lookup_vectors[1], (attention_group_count,), jnp.float32, 1.0 / 50.0, 1.0 / 20.0)
    slow_rate = jax.random.uniform(lookup_vectors[2], (attention_group_count,), jnp.float32, 0.1, 0.4) / STEP_COUNT_FULL
    ground_frequency = jnp.where(fast_heads, fast_rate, slow_rate)
    block_count = STEP_COUNT_FULL // TOK_DEV
    block_factor = jnp.exp(jax.random.uniform(lookup_vectors[3], (block_count, attention_group_count), jnp.float32, -0.7, 0.7))
    place_indices = jnp.repeat(block_factor, TOK_DEV, axis=0)
    noise_amplitude = jax.random.uniform(lookup_vectors[4], (STEP_COUNT_FULL, attention_group_count), jnp.float32, 0.5, 1.5)
    spike_place = jax.random.randint(lookup_vectors[5], (2,), 0, STEP_COUNT_FULL)
    spike_magnitude = jax.random.uniform(lookup_vectors[6], (2, attention_group_count), jnp.float32, 0.22, 0.69)
    spike_entry_indices = (jnp.arange(STEP_COUNT_FULL)[:, None] == spike_place[None, :]).astype(jnp.float32)
    return -(ground_frequency[None, :] * place_indices * noise_amplitude) - jnp.dot(spike_entry_indices, spike_magnitude)


def draw_decay_wide(key, part):
    return decay_draw(jax.random.fold_in(key, 11), HEADS_WIDE)


def draw_decay_narrow(key, part):
    return decay_draw(jax.random.fold_in(key, 23), HEADS_NARROW)


def level_of(rng, extent, shards, least, largest):
    loudness, own = 1.0, jax.random.fold_in(rng, 6)
    for position, parts in shards:
        draws = jnp.exp(jax.random.uniform(jax.random.fold_in(own, position), (parts,), jnp.float32, least / len(shards), largest / len(shards)))
        loudness = loudness * jnp.repeat(draws, extent[position] // parts).reshape([-1 if axis == position else 1 for axis in range(len(extent))])
    return loudness


def deal_out(own_key, own, number, rows, number_of, top, most, lean):
    order = jax.random.permutation(own_key, number_of)
    crowded, usual = load_shares(number_of, rows * top, most, lean, True), load_shares(number_of, rows * top, most, lean, False)
    places = jnp.arange(number_of)

    def named(lengths, offset_by):
        used = int((lengths > 0).sum())
        fixed = max(1, used // 4)
        shifted = fixed + (places - fixed + offset_by * (used - fixed)) % max(1, number_of - fixed)
        return jnp.zeros((number_of,), jnp.int32).at[order[jnp.where(places < fixed, places, shifted)]].set(jnp.asarray(lengths, jnp.int32))

    lengths = jnp.where(number % 4 == 0, named(crowded, number // 4), named(usual, number - number // 4 - 1))
    mixed = jax.random.permutation(jax.random.fold_in(own, 3), number_of)
    donor, taker = mixed[0:number_of // 2 * 2:2], mixed[1:number_of // 2 * 2:2]
    room = jnp.minimum(lengths[donor] - 1, most - lengths[taker]) // 2
    room = jnp.where((donor == order[0]) | (taker == order[0]) | (lengths[taker] == 0), 0, jnp.maximum(room, 0))
    shifted = jax.random.randint(jax.random.fold_in(own, 4), (number_of // 2,), 0, 1 << 20) % (room + 1)
    lengths = lengths.at[donor].add(-shifted).at[taker].add(shifted)
    members = jnp.searchsorted(jnp.cumsum(lengths), jnp.arange(rows * top), side="right").astype(jnp.int32)
    table = members.reshape(top, rows).T
    table = table[jax.random.permutation(jax.random.fold_in(own, 1), rows)]
    offset_by = jax.random.randint(jax.random.fold_in(own, 2), (rows, 1), 0, top)
    return jnp.take_along_axis(table, (jnp.arange(top)[None, :] + offset_by) % top, axis=1)


def load_shares(amount, total, limit, slope, full):
    weights = [(1 << 20) // math.isqrt(grade ** slope) + 1 for grade in range(1, amount + 1)]
    largest = limit if full else min(limit, max(-(-total // amount), total * weights[0] // sum(weights)))
    least = 1 if total - largest >= amount - 1 else 0
    counts, rest = [largest] + [least] * (amount - 1), total - largest - least * (amount - 1)
    while rest > 0:
        free = [i for i in range(1, amount) if counts[i] < largest] or [i for i in range(1, amount) if counts[i] < limit]
        pool, remaining = sum([weights[i] for i in free]), rest
        for i in free:
            extra = min(limit - counts[i], max(1, remaining * weights[i] // pool), rest)
            counts[i] = counts[i] + extra
            rest = rest - extra
    return np.array(counts)


def noise(key, shape, width, reach, cuts=(), kind=jnp.bfloat16):
    result = jax.random.normal(key, shape, jnp.float32) * width
    if len(cuts) > 0:
        result = level_of(key, shape, cuts, -0.22, 0.18) * result
    return jnp.clip(result, min=-reach, max=reach).astype(kind)


def setup_inputs(seed: int = 0, part: int = 0) -> dict:
    arg_keys = jax.random.split(jax.random.key(seed), 18)
    part_splits = jax.random.split(jax.random.fold_in(arg_keys[17], part), 18)
    query_wide = noise(part_splits[0], (STEP_COUNT_FULL, HEADS_WIDE * HEAD_WIDE), 1.0, 6.0, ((0, 32), (1, 4)))
    key_wide = noise(part_splits[1], (STEP_COUNT_FULL, HEADS_WIDE * HEAD_WIDE), 1.0, 6.0, ((0, 32), (1, 4)))
    value_wide = noise(part_splits[2], (STEP_COUNT_FULL, HEADS_WIDE * HEAD_WIDE), 1.0, 6.0, ((0, 32), (1, 4)))
    decay_wide = draw_decay_wide(jax.random.fold_in(jax.random.fold_in(arg_keys[17], part), 71), part)
    query_narrow = noise(part_splits[4], (STEP_COUNT_FULL, HEADS_NARROW * HEAD_NARROW), 1.0, 6.0, ((0, 32), (1, 4)))
    key_narrow = noise(part_splits[5], (STEP_COUNT_FULL, HEADS_NARROW * HEAD_NARROW), 1.0, 6.0, ((0, 32), (1, 4)))
    value_narrow = noise(part_splits[6], (STEP_COUNT_FULL, HEADS_NARROW * HEAD_NARROW), 1.0, 6.0, ((0, 32), (1, 4)))
    decay_narrow = draw_decay_narrow(jax.random.fold_in(jax.random.fold_in(arg_keys[17], part), 71), part)
    residual = noise(part_splits[8], (STEP_COUNT_FULL, D), 1.0, 6.0, ((0, 128),))
    out_wide = noise(arg_keys[9], (HEADS_WIDE * HEAD_WIDE, D), (HEADS_WIDE * HEAD_WIDE + HEADS_NARROW * HEAD_NARROW) ** -0.5, 0.125, ((0, 4),))
    out_narrow = noise(arg_keys[10], (HEADS_NARROW * HEAD_NARROW, D), (HEADS_WIDE * HEAD_WIDE + HEADS_NARROW * HEAD_NARROW) ** -0.5, 0.125, ((0, 4),))
    norm_gain = jnp.clip(1.0 + 0.18 * jax.random.normal(arg_keys[11], (D,), jnp.float32), 0.1, 1.9)
    routes_keys = jax.random.split(jax.random.fold_in(part_splits[12], 1), STEP_COUNT_FULL // ROWS_DEV)
    routes_turns = jax.random.permutation(jax.random.fold_in(part_splits[12], 3), STEP_COUNT_FULL // ROWS_DEV)
    routes = jax.vmap(lambda own, number: deal_out(jax.random.fold_in(part_splits[12], 2), own, number, ROWS_DEV, EXPERTS, TOP_K, CAPACITY, 1))(routes_keys, routes_turns).reshape((STEP_COUNT_FULL, TOP_K))
    route_weights = jnp.clip(jnp.exp(math.log(1.0) - 2.3025851 * jax.random.uniform(part_splits[13], (STEP_COUNT_FULL, TOP_K), jnp.float32) ** level_of(part_splits[13], (STEP_COUNT_FULL, TOP_K), ((0, 128),), -0.2, 0.2)), 0.1, 1.0)
    expert_gate = noise(arg_keys[14], (EXPERTS, D, FF), (D // 9) ** -0.5, 0.375, ((0, 32), (2, 4)))
    expert_up = noise(arg_keys[15], (EXPERTS, D, FF), (D // 9) ** -0.5, 0.375, ((0, 32), (2, 4)))
    expert_down = noise(arg_keys[16], (EXPERTS, FF, D), (FF * 16) ** -0.5, 0.03125, ((0, 32), (1, 4)))
    return {"query_wide": query_wide, "key_wide": key_wide, "value_wide": value_wide, "decay_wide": decay_wide, "query_narrow": query_narrow, "key_narrow": key_narrow, "value_narrow": value_narrow, "decay_narrow": decay_narrow, "residual": residual, "out_wide": out_wide, "out_narrow": out_narrow, "norm_gain": norm_gain, "routes": routes, "route_weights": route_weights, "expert_gate": expert_gate, "expert_up": expert_up, "expert_down": expert_down}


norm_eps = 1e-05
clamp_limit = 7.0
swish_alpha = 1.702
rotary_base = 10000.0
highest = lax.Precision.HIGHEST

def rotate(values, positions):
    half_width = values.shape[-1] // 2
    inverse = rotary_base ** (-jnp.arange(half_width, dtype=jnp.float32) / half_width)
    angles = positions[:, None] * inverse[None, :]
    cosine = jnp.cos(angles)[:, None, :]
    sine_part = jnp.sin(angles)[:, None, :]
    lower_half = values[..., :half_width]
    upper_half = values[..., half_width:]
    return jnp.concatenate([lower_half * cosine - upper_half * sine_part, lower_half * sine_part + upper_half * cosine], axis=-1)

def prepare(query_in, key_in, head_width, positions):
    length = query_in.shape[0]
    attention_group_count = query_in.shape[1] // head_width
    query_heads = query_in.astype(jnp.float32).reshape(length, attention_group_count, head_width)
    key_heads = key_in.astype(jnp.float32).reshape(length, attention_group_count, head_width)
    query_rot = rotate(query_heads, positions).astype(jnp.bfloat16)
    key_rot = (rotate(key_heads, positions) * head_width ** (-0.5)).astype(jnp.bfloat16)
    return (query_rot, key_rot)

def group_norm(output_heads):
    center = lax.optimization_barrier(jnp.mean(output_heads, axis=-1, keepdims=True))
    spread = lax.optimization_barrier(jnp.mean(jnp.square(output_heads - center), axis=-1, keepdims=True))
    return (output_heads - center) * lax.rsqrt(spread + norm_eps)

def block_terms(query_f, key_f, value_f, log_decay):
    block_len = query_f.shape[0]
    cumulative = jnp.cumsum(log_decay, axis=0)
    steps_in = jnp.arange(block_len, dtype=jnp.int32)
    causal = steps_in[:, None] >= steps_in[None, :]
    gaps = cumulative.T[:, :, None] - cumulative.T[:, None, :]
    decay_grid = jnp.exp(jnp.where(causal[None], gaps, -jnp.inf))
    scores = jnp.einsum('thd,shd->hts', query_f, key_f, precision=highest) * decay_grid
    inner_part = jnp.einsum('hts,she->the', scores, value_f, precision=highest)
    total_log = cumulative[-1]
    weighted = key_f * jnp.exp(total_log[None, :] - cumulative)[:, :, None]
    state_local = jnp.einsum('shd,she->hde', weighted, value_f, precision=highest)
    return (inner_part, cumulative, total_log, state_local)

def read_carried(query_f, cumulative, state_in):
    return jnp.exp(cumulative)[:, :, None] * jnp.einsum('thd,hde->the', query_f, state_in, precision=highest)

def retain(query_in, key_in, value_in, log_decay, head_width):
    length = query_in.shape[0]
    attention_group_count = query_in.shape[1] // head_width
    positions = jnp.arange(length, dtype=jnp.float32)
    query_rot, key_rot = prepare(query_in, key_in, head_width, positions)
    block_len = math.gcd(length, 128)
    blocks = length // block_len

    def advance(state_now, inputs):
        query_block, key_block, value_block, decay_block = inputs
        query_f = query_block.astype(jnp.float32)
        key_f = key_block.astype(jnp.float32)
        value_f = value_block.astype(jnp.float32)
        inner_part, cumulative, total_log, state_local = block_terms(query_f, key_f, value_f, decay_block)
        output_block = inner_part + read_carried(query_f, cumulative, state_now)
        state_next = jnp.exp(total_log)[:, None, None] * state_now + state_local
        return (state_next, output_block)
    value_heads = value_in.reshape(length, attention_group_count, head_width)
    inputs = (query_rot.reshape(blocks, block_len, attention_group_count, head_width), key_rot.reshape(blocks, block_len, attention_group_count, head_width), value_heads.reshape(blocks, block_len, attention_group_count, head_width), log_decay.reshape(blocks, block_len, attention_group_count))
    final_state, outputs = lax.scan(advance, jnp.zeros((attention_group_count, head_width, head_width), jnp.float32), inputs)
    normed_heads = group_norm(outputs.reshape(length, attention_group_count, head_width))
    return normed_heads.reshape(length, attention_group_count * head_width).astype(jnp.bfloat16)

def activate(gate_pre, up_pre):
    gate_clip = jnp.minimum(gate_pre, clamp_limit)
    up_clip = jnp.clip(up_pre, -clamp_limit, clamp_limit)
    return gate_clip * jax.nn.sigmoid(swish_alpha * gate_clip) * (up_clip + 1.0)

def round_trip(values):
    return lax.optimization_barrier(values.astype(jnp.bfloat16)).astype(jnp.float32)

def moe_reference(normed, routes, route_weights, expert_gate, expert_up, expert_down):
    length = normed.shape[0]
    slot_count = N_SP * N_TP * CAPACITY
    padded = jnp.concatenate([normed, jnp.zeros((1, D), jnp.bfloat16)], axis=0)

    def per_expert(total_rows, inputs):
        expert_index, gate_w, up_w, down_w = inputs
        chosen = routes == expert_index
        hits = jnp.any(chosen, axis=1).astype(jnp.int32)
        weight = lax.optimization_barrier(jnp.sum(jnp.where(chosen, route_weights, 0.0), axis=1))
        weight_pad = jnp.concatenate([weight, jnp.zeros((1,), jnp.float32)])
        rank_in = jnp.cumsum(hits) - hits
        target = jnp.where(hits > 0, rank_in, slot_count).astype(jnp.int32)
        slot_table = jnp.full((slot_count + 1,), length, jnp.int32).at[target].set(jnp.arange(length, dtype=jnp.int32))[:slot_count]
        slot_rows = padded[slot_table]
        gate_pre = jnp.dot(slot_rows, gate_w, preferred_element_type=jnp.float32)
        up_pre = jnp.dot(slot_rows, up_w, preferred_element_type=jnp.float32)
        hidden = activate(gate_pre, up_pre).astype(jnp.bfloat16)
        pieces = hidden.reshape(slot_count, N_TP, FF // N_TP).astype(jnp.float32)
        down_parts = down_w.reshape(N_TP, FF // N_TP, D).astype(jnp.float32)
        partial_value = jnp.einsum('nqf,qfd->qnd', pieces, down_parts)
        summed = lax.optimization_barrier(jnp.sum(round_trip(partial_value), axis=0))
        expert_output = summed.astype(jnp.bfloat16).astype(jnp.float32)
        contrib = expert_output * weight_pad[slot_table][:, None]
        return (total_rows.at[slot_table].add(contrib), None)
    total_rows, unused = lax.scan(per_expert, jnp.zeros((length + 1, D), jnp.float32), (jnp.arange(EXPERTS, dtype=jnp.int32), expert_gate, expert_up, expert_down))
    return total_rows[:length]

def reference(query_wide, key_wide, value_wide, decay_wide, query_narrow, key_narrow, value_narrow, decay_narrow, residual, out_wide, out_narrow, norm_gain, routes, route_weights, expert_gate, expert_up, expert_down):
    mixed_wide = retain(query_wide, key_wide, value_wide, decay_wide, HEAD_WIDE)
    mixed_narrow = retain(query_narrow, key_narrow, value_narrow, decay_narrow, HEAD_NARROW)
    wide_share = HEADS_WIDE * HEAD_WIDE // N_TP
    narrow_share = HEADS_NARROW * HEAD_NARROW // N_TP
    attention = jnp.zeros((STEP_COUNT_FULL, D), jnp.float32)
    for tp_part in range(N_TP):
        wide_cols = slice(tp_part * wide_share, (tp_part + 1) * wide_share)
        narrow_cols = slice(tp_part * narrow_share, (tp_part + 1) * narrow_share)
        partial_value = jnp.dot(mixed_wide[:, wide_cols], out_wide[wide_cols], preferred_element_type=jnp.float32)
        partial_value = partial_value + jnp.dot(mixed_narrow[:, narrow_cols], out_narrow[narrow_cols], preferred_element_type=jnp.float32)
        attention = attention + round_trip(partial_value)
    hidden_state = residual.astype(jnp.float32) + attention
    scale_row = lax.rsqrt(lax.optimization_barrier(jnp.mean(hidden_state * hidden_state, axis=-1, keepdims=True)) + norm_eps)
    normed = (hidden_state * scale_row * norm_gain).astype(jnp.bfloat16)
    routed = moe_reference(normed, routes, route_weights, expert_gate, expert_up, expert_down)
    return (hidden_state + routed).astype(jnp.bfloat16)
```

```python
import jax
import jax.numpy as jnp
import numpy as np
from jax import lax
from jax.experimental import pallas as pl
from jax.experimental.pallas import tpu as pltpu
from jax.sharding import Mesh
from jax.sharding import PartitionSpec as P

HEAD_WIDE = 128
HEAD_NARROW = 64
TOP_K = 2
SP = ("z", "c")
GRP_SP = ("grp", "z", "c")
GRP_SP_TP = ("grp", "z", "c", "tp")
CHUNK = 4
PAY = 208

norm_eps = 1e-05
clamp_limit = 7.0
swish_alpha = 1.702
rotary_base = 10000.0

f32 = jnp.float32
bf16 = jnp.bfloat16
HIGH = lax.Precision.HIGHEST


def iota(shape, dim):
    return lax.broadcasted_iota(jnp.int32, shape, dim)


def dot(a, b, dims=((1,), (0,)), precision=None):
    return lax.dot_general(a, b, (dims, ((), ())), precision=precision, preferred_element_type=f32)


def kernel_call(body, out_shape, n_in, scalars=0, scratch=(), **kw):
    vm = pl.BlockSpec(memory_space=pltpu.VMEM)
    sm = pl.BlockSpec(memory_space=pltpu.SMEM)
    return pl.pallas_call(
        body,
        out_shape=out_shape,
        in_specs=[sm] * scalars + [vm] * n_in,
        out_specs=jax.tree.map(lambda _: vm, out_shape),
        scratch_shapes=list(scratch),
        **kw,
    )


def rotary_tables(length, n_sp):
    wide = rotary_base ** (-np.arange(64) / 64.0)
    narrow = rotary_base ** (-np.arange(32) / 32.0)
    freq = np.concatenate([wide, wide, narrow, narrow, narrow, narrow])
    rows = []
    for count, step in ((n_sp, length), (length // 32, 32), (32, 1)):
        angle = (np.arange(count) * step)[:, None] * freq[None, :]
        rows += [np.cos(angle), np.sin(angle)]
    return np.concatenate(rows).astype(np.float32)


def local_kernel(length, n_sp):
    coarse = length // 32

    def body(ids, tab, qw, kw, qn, kn, vw, vn, dc, dr, qr_out, kr_out, lc_out, lr_out, keep_out, send_out, cs, sn, st):
        sp, core = ids[0], ids[1]
        bc, bs = tab[pl.ds(sp, 1), :], tab[pl.ds(n_sp + sp, 1), :]
        o = 2 * n_sp
        ac, as_ = tab[o : o + coarse, :], tab[o + coarse : o + 2 * coarse, :]
        o = o + 2 * coarse
        fc, fs = tab[o : o + 32, :], tab[o + 32 : o + 64, :]
        a2c = ac * bc - as_ * bs
        a2s = as_ * bc + ac * bs
        lane = iota((1, 256), 1)
        inside = jnp.where(lane < 128, lane % 128 - 64, lane % 64 - 32)
        sign = jnp.where(inside < 0, -1.0, 1.0).astype(f32)
        for a in range(coarse):
            cs[32 * a : 32 * a + 32, :] = a2c[a : a + 1] * fc - a2s[a : a + 1] * fs
            sn[32 * a : 32 * a + 32, :] = (a2s[a : a + 1] * fc + a2c[a : a + 1] * fs) * sign
        lane128 = iota((length, 128), 1)
        low32 = lane128 % 64 < 32
        low64 = lane128 < 64

        def turned(x, narrow):
            x = x.astype(f32)
            if narrow:
                other = jnp.where(low32, pltpu.roll(x, 96, 1), pltpu.roll(x, 32, 1))
                return x * cs[:, 128:] + other * sn[:, 128:]
            return x * cs[:, :128] + pltpu.roll(x, 64, 1) * sn[:, :128]

        tri = (iota((length, length), 0) >= iota((length, length), 1)).astype(f32)
        lc = dot(tri, dc[...], precision=HIGH)
        lr = dot(dr[...], tri, ((1,), (1,)), precision=HIGH)
        lc_out[...] = lc
        lr_out[...] = lr
        total = lc[length - 1 : length, :]
        to_end = jnp.exp(total - lc)
        row128 = iota((1, 128), 1)
        for g in range(4):
            narrow, h = g >= 2, g % 2
            q_in, k_in, v_in = (qn, kn, vn) if narrow else (qw, kw, vw)
            part = slice(h * 128, h * 128 + 128)
            width = HEAD_NARROW if narrow else HEAD_WIDE
            qr_out[:, g * 128 : g * 128 + 128] = turned(q_in[:, part], narrow).astype(bf16)
            key = (turned(k_in[:, part], narrow) * width ** (-0.5)).astype(bf16)
            kr_out[:, g * 128 : g * 128 + 128] = key
            if narrow:
                a = 2 + 2 * h
                left = jnp.where(low64, to_end[:, a : a + 1], to_end[:, a + 1 : a + 2])
                log = jnp.where(row128 < 64, total[:, a : a + 1], total[:, a + 1 : a + 2])
            else:
                left = to_end[:, h : h + 1]
                log = jnp.broadcast_to(total[:, h : h + 1], (1, 128))
            weighted = (key.astype(f32) * left).astype(bf16)
            state = dot(weighted, v_in[:, part], ((0,), (0,)))
            if narrow:
                st[h, 128:192, :] = jnp.where(iota((64, 128), 1) < 64, state[:64], state[64:])
            else:
                st[h, 0:128, :] = state
            put_log(st.at[h], log, narrow)
        keep = jnp.where(core == 0, st[0], st[1])
        send = jnp.where(core == 0, st[1], st[0])
        keep_out[...] = keep.astype(bf16)
        send_out[...] = send.astype(bf16)

    return kernel_call(
        body,
        (
            jax.ShapeDtypeStruct((length, 512), bf16),
            jax.ShapeDtypeStruct((length, 512), bf16),
            jax.ShapeDtypeStruct((length, 8), f32),
            jax.ShapeDtypeStruct((8, length), f32),
            jax.ShapeDtypeStruct((PAY, 128), bf16),
            jax.ShapeDtypeStruct((PAY, 128), bf16),
        ),
        9,
        scalars=1,
        scratch=(
            pltpu.VMEM((length, 256), f32),
            pltpu.VMEM((length, 256), f32),
            pltpu.VMEM((2, PAY, 128), f32),
        ),
        name="local_terms",
    )


def put_log(ref, log, narrow):
    hi = log.astype(bf16).astype(f32)
    mid = (log - hi).astype(bf16).astype(f32)
    low = log - hi - mid
    row = iota((8, 128), 0)
    block = jnp.where(row == 0, hi, jnp.where(row == 1, mid, jnp.where(row == 2, low, 0.0)))
    at = 200 if narrow else 192
    ref[at : at + 8, :] = block


def log_rows(pay):
    wide = pay[192:193] + pay[193:194] + pay[194:195]
    narrow = pay[200:201] + pay[201:202] + pay[202:203]
    return wide, narrow


def decayed(pay, state):
    wide, narrow = log_rows(pay)
    row = iota((192, 128), 0)
    return jnp.where(row < 128, jnp.exp(wide), jnp.exp(narrow)) * state


def pair_kernel():
    def body(ids, keep, got, out, st):
        core = ids[1]
        own, other = keep[...].astype(f32), got[...].astype(f32)
        first = jnp.where(core == 0, own, other)
        second = jnp.where(core == 0, other, own)
        st[0:192, :] = decayed(second, first[0:192]) + second[0:192]
        fw, fn = log_rows(first)
        sw, sn = log_rows(second)
        put_log(st, fw + sw, False)
        put_log(st, fn + sn, True)
        out[...] = st[...].astype(bf16)

    return kernel_call(
        body, jax.ShapeDtypeStruct((PAY, 128), bf16), 2, scalars=1,
        scratch=(pltpu.VMEM((PAY, 128), f32),), name="pair_total",
    )


def prefix_kernel(n_z):
    def body(ids, pieces, keep, got, mine_out, other_out):
        core, z = ids[1], ids[2]

        def step(k, acc):
            pay = pieces[k].astype(f32)
            new = decayed(pay, acc) + pay[0:192]
            return jnp.where(k < z, new, acc)

        before = lax.fori_loop(0, n_z, step, jnp.zeros((192, 128), f32))
        first = jnp.where(core == 0, keep[...].astype(f32), got[...].astype(f32))
        after = decayed(first, before) + first[0:192]
        mine_out[...] = jnp.where(core == 0, before, after).astype(bf16)
        other_out[...] = jnp.where(core == 0, after, before).astype(bf16)

    return kernel_call(
        body,
        (jax.ShapeDtypeStruct((192, 128), bf16), jax.ShapeDtypeStruct((192, 128), bf16)),
        3, scalars=1, name="prefix_states",
    )


def inner_kernel(length):
    nb = length // 128

    def body(qr, kr, vw, vn, lc, lr, out):
        causal = iota((128, 128), 0) >= iota((128, 128), 1)
        low = iota((128, 128), 1) < 64
        for g in range(4):
            narrow = g >= 2
            lanes = slice(g * 128, g * 128 + 128)
            v_in = vn if narrow else vw
            vl = slice((g % 2) * 128, (g % 2) * 128 + 128)
            heads = (2 + 2 * (g % 2), 3 + 2 * (g % 2)) if narrow else (g,)
            for i in range(nb):
                rows = slice(i * 128, i * 128 + 128)
                n = (i + 1) * 128
                results = []
                for n_head, h in enumerate(heads):
                    q = qr[rows, lanes]
                    if narrow:
                        keep = low if n_head == 0 else jnp.logical_not(low)
                        q = jnp.where(keep, q.astype(f32), 0.0).astype(bf16)
                    scores = dot(q, kr[0:n, lanes], ((1,), (1,)))
                    gaps = lc[rows, h : h + 1] - lr[h : h + 1, 0:n]
                    if i == 0:
                        grid = jnp.where(causal, gaps, -jnp.inf)
                    else:
                        grid = jnp.concatenate(
                            [gaps[:, : n - 128], jnp.where(causal, gaps[:, n - 128 :], -jnp.inf)], axis=1
                        )
                    scores = (scores * jnp.exp(grid)).astype(bf16)
                    results.append(dot(scores, v_in[0:n, vl]))
                out[rows, lanes] = jnp.where(low, results[0], results[1]) if narrow else results[0]

    return kernel_call(body, jax.ShapeDtypeStruct((length, 512), f32), 6, name="inner_terms")


def mixed_kernel(length, parts, width):
    rows_dev = length // parts

    def body(ids, qr, lc, inner, mine, got, ow, on, out):
        core = ids[1]
        own, other = mine[...].astype(f32), got[...].astype(f32)
        halves = (jnp.where(core == 0, own, other), jnp.where(core == 0, other, own))
        low = iota((1, 128), 1) < 64
        grow = jnp.exp(lc[...])
        mixed = []
        for g in range(4):
            lanes = slice(g * 128, g * 128 + 128)
            half = halves[g % 2]
            if g < 2:
                state = half[0:128]
                scale = grow[:, g : g + 1]
            else:
                block = half[128:192]
                state = jnp.concatenate([jnp.where(low, block, 0.0), jnp.where(low, 0.0, block)], axis=0)
                a = 2 + 2 * (g % 2)
                scale = jnp.where(low, grow[:, a : a + 1], grow[:, a + 1 : a + 2])
            x = inner[:, lanes] + scale * dot(qr[:, lanes], state.astype(bf16))
            if g < 2:
                x = x - jnp.mean(x, axis=1, keepdims=True)
                spread = jnp.mean(x * x, axis=1, keepdims=True)
            else:
                every = jnp.sum(x, axis=1, keepdims=True)
                left = jnp.sum(jnp.where(low, x, 0.0), axis=1, keepdims=True)
                x = x - jnp.where(low, left, every - left) * (1.0 / 64.0)
                sq = x * x
                left = jnp.sum(jnp.where(low, sq, 0.0), axis=1, keepdims=True)
                right = jnp.sum(jnp.where(low, 0.0, sq), axis=1, keepdims=True)
                spread = jnp.where(low, left, right) * (1.0 / 64.0)
            mixed.append((x * lax.rsqrt(spread + norm_eps)).astype(bf16))
        wide = jnp.concatenate(mixed[:2], axis=1)
        narrow = jnp.concatenate(mixed[2:], axis=1)
        for j in range(parts):
            rows = slice(j * rows_dev, (j + 1) * rows_dev)
            out[j] = (dot(wide[rows], ow[...]) + dot(narrow[rows], on[...])).astype(bf16)

    return kernel_call(
        body, jax.ShapeDtypeStruct((parts, rows_dev, width), bf16), 7, scalars=1, name="mixed_out"
    )


def norm_kernel(rows_dev, width):
    def body(parts, residual, gain, hidden_out, normed_out):
        x = residual[...].astype(f32)
        attention = parts[0].astype(f32)
        for j in range(1, parts.shape[0]):
            attention = attention + parts[j].astype(f32)
        x = x + attention
        hidden_out[...] = x
        scale = lax.rsqrt(jnp.mean(x * x, axis=1, keepdims=True) + norm_eps)
        normed_out[...] = (x * scale * gain[...]).astype(bf16)

    return kernel_call(
        body,
        (jax.ShapeDtypeStruct((rows_dev, width), f32), jax.ShapeDtypeStruct((rows_dev, width), bf16)),
        3,
        name="hidden_norm",
    )


def dispatch_kernel(rows_dev, width, n_z, chunks):
    tokens = 2 * rows_dev
    slots = n_z * 2 * CHUNK

    def body(ids, own, got, rr, *refs):
        outs, rows_ref = refs[:chunks], refs[chunks]
        core = ids[1]
        rows_ref[0:rows_dev, :] = own[...]
        rows_ref[rows_dev:tokens, :] = got[...]
        experts = 2 * n_z
        expert = iota((experts, tokens), 0).astype(f32)
        named = jnp.logical_or(rr[0:1, :] == expert, rr[1:2, :] == expert)
        t0, t1 = iota((tokens, tokens), 0), iota((tokens, tokens), 1)
        ahead = jnp.logical_and(t0 < t1, t0 // rows_dev == t1 // rows_dev)
        rank = dot(named.astype(f32).astype(bf16), ahead.astype(f32).astype(bf16))
        table = jnp.where(named, rank, -1.0).astype(bf16)
        spread = (iota((slots, experts), 1) == 2 * (iota((slots, experts), 0) // (2 * CHUNK)) + core)
        ranks = dot(spread.astype(f32).astype(bf16), table)
        row = iota((slots, tokens), 0)
        same = (row % (2 * CHUNK)) // CHUNK == iota((slots, tokens), 1) // rows_dev
        slot = (row % CHUNK).astype(f32)
        for k in range(chunks):
            pick = jnp.logical_and(same, ranks == slot + float(k * CHUNK)).astype(f32).astype(bf16)
            outs[k][...] = dot(pick, rows_ref[...]).astype(bf16)

    return kernel_call(
        body,
        tuple(jax.ShapeDtypeStruct((slots, width), bf16) for _ in range(chunks)),
        3, scalars=1, scratch=(pltpu.VMEM((tokens, width), bf16),), name="dispatch_rows",
    )


def combine_kernel(rows_dev, width, n_z, chunks):
    tokens = 2 * rows_dev
    slots = n_z * 2 * CHUNK

    def body(ids, rc, *refs):
        back, own_out, other_out = refs[:chunks], refs[chunks], refs[chunks + 1]
        core = ids[1]
        experts = 2 * n_z
        expert = iota((tokens, experts), 1).astype(f32)
        named = [rc[:, k : k + 1] == expert for k in range(TOP_K)]
        t0, t1 = iota((tokens, tokens), 0), iota((tokens, tokens), 1)
        behind = jnp.logical_and(t1 < t0, t0 // rows_dev == t1 // rows_dev)
        either = jnp.logical_or(named[0], named[1]).astype(f32).astype(bf16)
        rank = dot(behind.astype(f32).astype(bf16), either)
        lane = iota((tokens, slots), 1)
        same = (lane % (2 * CHUNK)) // CHUNK == iota((tokens, slots), 0) // rows_dev
        lane_expert = (2 * (lane // (2 * CHUNK)) + core).astype(f32)
        slot = (lane % CHUNK).astype(f32)
        total = None
        for k in range(TOP_K):
            mine = jnp.sum(jnp.where(named[k], rank, 0.0), axis=1, keepdims=True)
            hit = jnp.logical_and(same, lane_expert == rc[:, k : k + 1])
            picked = None
            for n in range(chunks):
                pick = jnp.logical_and(hit, mine == slot + float(n * CHUNK)).astype(f32).astype(bf16)
                term = dot(pick, back[n][...])
                picked = term if picked is None else picked + term
            term = picked * rc[:, TOP_K + k : TOP_K + k + 1]
            total = term if total is None else total + term
        own_out[...] = total[0:rows_dev]
        other_out[...] = total[rows_dev:tokens].astype(bf16)

    return kernel_call(
        body,
        (jax.ShapeDtypeStruct((rows_dev, width), f32), jax.ShapeDtypeStruct((rows_dev, width), bf16)),
        1 + chunks, scalars=1, name="combine_rows",
    )


def experts_kernel(rows, width, ff, steps):
    sizes = (rows, rows, rows, rows // 2, rows // 2)
    total = sum(sizes)
    block = ff // steps

    def body(*refs):
        ins, (gate, up, down), outs, (x, acc) = refs[:5], refs[5:8], refs[8:13], refs[13:]
        step = pl.program_id(0)

        @pl.when(step == 0)
        def _():
            at = 0
            for ref, size in zip(ins, sizes):
                x[at : at + size, :] = ref[...]
                at += size

        gate_clip = jnp.minimum(dot(x[...], gate[...]), clamp_limit)
        up_clip = jnp.clip(dot(x[...], up[...]), -clamp_limit, clamp_limit)
        hidden = (gate_clip * jax.nn.sigmoid(swish_alpha * gate_clip) * (up_clip + 1.0)).astype(bf16)
        term = dot(hidden, down[...])

        @pl.when(step == 0)
        def _():
            acc[...] = term

        @pl.when(step > 0)
        def _():
            acc[...] += term

        @pl.when(step == steps - 1)
        def _():
            at = 0
            for ref, size in zip(outs, sizes):
                ref[...] = acc[at : at + size, :].astype(bf16)
                at += size

    whole = [pl.BlockSpec((size, width), lambda j: (0, 0)) for size in sizes]
    return pl.pallas_call(
        body,
        grid=(steps,),
        in_specs=whole
        + [
            pl.BlockSpec((width, block), lambda j: (0, j)),
            pl.BlockSpec((width, block), lambda j: (0, j)),
            pl.BlockSpec((block, width), lambda j: (j, 0)),
        ],
        out_specs=whole,
        out_shape=[jax.ShapeDtypeStruct((size, width), bf16) for size in sizes],
        scratch_shapes=[pltpu.VMEM((total, width), bf16), pltpu.VMEM((total, width), f32)],
        cost_estimate=pl.CostEstimate(
            flops=6 * total * width * ff, bytes_accessed=6 * width * ff + 4 * total * width, transcendentals=total * ff
        ),
        name="expert_rows",
    )


def shift(value, axis, by):
    n = lax.axis_size(axis)
    return lax.ppermute(value, axis, [(i, (i + by) % n) for i in range(n)])


def after(value, *others):
    return lax.optimization_barrier((value, *others))[0]


def x_gather(own):
    half = own.shape[0] // 2
    left, right = shift(own, "tp", 1), shift(own, "tp", -1)
    far_top = shift(left[:half], "tp", 1)
    far_low = shift(right[half:], "tp", -1)
    return own, left, right, far_top, far_low


def x_scatter(own, left, right, far_top, far_low):
    half = far_top.shape[0]
    top, low = shift(far_top, "tp", 1), shift(far_low, "tp", -1)
    right = jnp.concatenate([(right[:half].astype(f32) + top.astype(f32)).astype(bf16), right[half:]])
    left = jnp.concatenate([left[:half], (left[half:].astype(f32) + low.astype(f32)).astype(bf16)])
    a, b = shift(right, "tp", 1), shift(left, "tp", -1)
    return (own.astype(f32) + a.astype(f32) + b.astype(f32)).astype(bf16)


def body(
    query_wide, key_wide, value_wide, decay_wide, query_narrow, key_narrow, value_narrow, decay_narrow,
    residual, out_wide, out_narrow, norm_gain, routes, route_weights, expert_gate, expert_up, expert_down,
):
    length = query_wide.shape[0]
    tp_count = lax.axis_size("tp")
    n_z, n_sp = lax.axis_size("z"), lax.axis_size(SP)
    rows_dev, width = residual.shape
    ff = expert_gate.shape[2]
    capacity = max(2, 3 * rows_dev * TOP_K // (2 * n_sp))
    chunks = -(-capacity // CHUNK)
    ids = jnp.stack([lax.axis_index(SP), lax.axis_index("c"), lax.axis_index("z")]).astype(jnp.int32)

    table = jnp.asarray(rotary_tables(length, n_sp))
    decay = jnp.concatenate([decay_wide, decay_narrow, jnp.zeros((length, 2), f32)], axis=1)
    qr, kr, lc, lr, keep, send = local_kernel(length, n_sp)(
        ids, table, query_wide, key_wide, query_narrow, key_narrow, value_wide, value_narrow, decay, decay.T
    )
    got = shift(send, "c", 1)
    total = pair_kernel()(ids, keep, got)
    pieces = lax.all_gather(total, "z")
    inner = inner_kernel(length)(qr, kr, value_wide, value_narrow, lc, lr)
    route_cols = jnp.concatenate([routes.astype(f32), route_weights], axis=1)
    route_cols = jnp.concatenate([route_cols, shift(route_cols, "c", 1)], axis=0)
    route_cols = jnp.pad(route_cols, ((0, 0), (0, 4)))
    route_rows = route_cols.T
    mine, other = prefix_kernel(n_z)(ids, pieces, keep, got)
    other = shift(other, "c", 1)
    parts = mixed_kernel(length, tp_count, width)(ids, qr, lc, inner, mine, other, out_wide, out_narrow)
    parts = lax.all_to_all(parts, "tp", 0, 0, tiled=True)
    hidden, normed = norm_kernel(rows_dev, width)(parts, residual, norm_gain.reshape(1, width))
    normed_got = shift(normed, "c", 1)
    sends = dispatch_kernel(rows_dev, width, n_z, chunks)(ids, normed, normed_got, route_rows)

    def over_z(value):
        value = value.reshape(n_z, 2 * CHUNK, width)
        return lax.all_to_all(value, "z", 0, 0, tiled=True).reshape(n_z * 2 * CHUNK, width)

    run = experts_kernel(n_z * 2 * CHUNK, width, ff, 2)
    arrived, prev = [], None
    for k in range(chunks):
        value = sends[k] if prev is None else after(sends[k], prev)
        prev = over_z(value)
        arrived.append(prev)
    back = []
    for k in range(chunks):
        results = run(*x_gather(arrived[k]), expert_gate[0], expert_up[0], expert_down[0])
        summed = after(x_scatter(*results), prev)
        prev = over_z(summed)
        back.append(prev)
    part, part_other = combine_kernel(rows_dev, width, n_z, chunks)(ids, route_cols, *back)
    part_got = shift(part_other, "c", 1)
    return (hidden + part + part_got.astype(f32)).astype(bf16)


def solution(mesh):
    torus = Mesh(
        mesh.devices.reshape(mesh.shape["grp"], mesh.shape["sp"] // 2, 2, mesh.shape["tp"]),
        ("grp", "z", "c", "tp"),
    )
    rows, cols = P(GRP_SP, "tp"), P("tp", None)
    tokens = P(GRP_SP_TP, None)
    in_specs = (rows,) * 8 + (tokens, cols, cols, P(), tokens, tokens) + (
        P(SP, None, "tp"), P(SP, None, "tp"), P(SP, "tp", None),
    )
    return jax.shard_map(body, mesh=torus, in_specs=in_specs, out_specs=tokens, check_vma=False)
```
